32 devices in a mesh: grp: 2 (over x), tp: 4 (over y, core), dp: 4 (over z).
Axes of the slice: x: 2, y: 2, z: 4, core: 2. Of those that a mesh axis runs over, the one named last changes fastest.
Arguments:
- tokens: bfloat16 [64, 4096], P(('grp', 'tp'), 'dp'), parts along dimension 0, may hold values from -45 to 45
- w_in: bfloat16 [2, 2, 4096, 8192], P(None, None, 'dp', 'tp'), may hold values from -0.09375 to 0.09375
- w_vec: bfloat16 [2, 2, 4096, 2048], P(None, None, 'dp', 'tp'), may hold values from -0.09375 to 0.09375
- w_step: bfloat16 [2, 4096, 128], P(None, 'dp'), may hold values from -0.09375 to 0.09375
- conv_weight: bfloat16 [2, 4, 8192], P(None, None, 'tp'), may hold values from -3 to 3
- conv_vec: bfloat16 [2, 2, 4, 2048], P(None, None, None, 'tp'), may hold values from -3 to 3
- conv_state: bfloat16 [2, 64, 3, 8192], P(None, ('grp', 'dp'), None, 'tp'), parts along dimension 1, may hold values from -6 to 6
- vec_state: bfloat16 [2, 2, 64, 3, 2048], P(None, None, ('grp', 'dp'), None, 'tp'), parts along dimension 2, may hold values from -6 to 6
- ssm_state: float32 [2, 64, 128, 64, 128], P(None, ('grp', 'dp'), 'tp'), parts along dimension 1, may hold values from -4 to 4
- step_bias: float32 [2, 128], P(None, 'tp'), may hold values from -1.5 to 1
- decay_log: float32 [2, 128], P(None, 'tp'), may hold values from -4 to 1
- skip_gain: float32 [2, 128], P(None, 'tp'), may hold values from 0.5 to 3
- mix_gain: bfloat16 [2, 4096], P(None, 'dp'), may hold values from 0.099609375 to 1.8984375
- out_gain: bfloat16 [2, 8192], P(None, 'tp'), may hold values from 0.099609375 to 1.8984375
- w_out: bfloat16 [2, 8192, 4096], P(None, 'tp', 'dp'), may hold values from -0.0625 to 0.0625
Outputs:
- new_tokens: bfloat16 [64, 4096], P(('grp', 'tp'), 'dp'), parts along dimension 0
- new_conv: bfloat16 [2, 64, 3, 8192], P(None, ('grp', 'dp'), None, 'tp'), parts along dimension 1
- new_vec: bfloat16 [2, 2, 64, 3, 2048], P(None, None, ('grp', 'dp'), None, 'tp'), parts along dimension 2
- new_ssm: float32 [2, 64, 128, 64, 128], P(None, ('grp', 'dp'), 'tp'), parts along dimension 1
The draws below stay inside these ranges and needn't reach their ends.
There are 2 independent parts, one for each index of `grp`. The reference program is written for one: setup_inputs(seed, part) draws one part's arguments, and reference() takes and returns one part's arrays. A program takes and returns all parts, laid end to end along the dimension named above; an argument that names none is the same for every part. Nothing has to cross between parts.
All inputs are finite; a program needn't handle non-finite values.
Results may differ from the reference program's by a relative error of at most 0.023.
Values may be sent and summed in bfloat16 or wider, within the bound.
No kernel may reach another device: no remote copies, remote signals or barrier semaphores. Data moves between devices by JAX's collectives and lax.ppermute only.
A program may use at most 128 MiB of HBM per device.

```python
import jax
import jax.numpy as jnp
from jax import lax

MODEL_WIDTH = 4096
HEAD_COUNT = 128
HEAD_DIM = 64
STATE_DIM = 128
GROUP_COUNT = 16
CONV_TAPS = 4
LAYER_COUNT = 2
INNER_WIDTH = 8192
VEC_WIDTH = 2048
BATCH_SEQS = 32


def draw_tokens(key, part):
    base_key = jax.random.fold_in(key, 17)
    key_base, key_row = jax.random.split(base_key, 2)
    columns = jnp.exp(jnp.linspace(jnp.log(0.4), jnp.log(2.4), MODEL_WIDTH)).astype(jnp.float32)
    row_scale = jnp.exp(jax.random.uniform(key_row, (BATCH_SEQS, 1), jnp.float32, 0.0, jnp.log(10.0)))
    base = jnp.clip(jax.random.normal(key_base, (BATCH_SEQS, MODEL_WIDTH), jnp.float32), -6.0, 6.0)
    return (0.3 * base * columns[None, :] * row_scale).astype(jnp.bfloat16)


def levels(rng, extent, shards, low, largest):
    factor_of = 1.0
    for axis_at, parts in shards:
        heights = jax.random.uniform(jax.random.fold_in(jax.random.fold_in(rng, 6), axis_at), (parts,), jnp.float32, low / len(shards), largest / len(shards))
        factor_of = factor_of * jnp.repeat(jnp.exp(heights), extent[axis_at] // parts).reshape((-1,) + (1,) * (len(extent) - 1 - axis_at))
    return factor_of


def bell_draw(rng, extent, width, bound, cuts=(), dtype=jnp.bfloat16):
    values = width * jax.random.normal(rng, extent, jnp.float32)
    if cuts:
        values = values * levels(rng, extent, cuts, -0.22, 0.18)
    return jnp.clip(values, -bound, bound).astype(dtype)


def setup_inputs(seed: int = 0, part: int = 0) -> dict:
    key_of = jax.random.split(jax.random.key(seed), 16)
    part_splits = jax.random.split(jax.random.fold_in(key_of[15], part), 16)
    return {
        "tokens": draw_tokens(jax.random.fold_in(jax.random.fold_in(key_of[15], part), 71), part),
        "w_in": bell_draw(key_of[1], (LAYER_COUNT, 2, MODEL_WIDTH, INNER_WIDTH), MODEL_WIDTH ** -0.5, 0.09375, ((2, 4), (3, 4))),
        "w_vec": bell_draw(key_of[2], (LAYER_COUNT, 2, MODEL_WIDTH, VEC_WIDTH), MODEL_WIDTH ** -0.5, 0.09375, ((2, 4), (3, 4))),
        "w_step": bell_draw(key_of[3], (LAYER_COUNT, MODEL_WIDTH, HEAD_COUNT), MODEL_WIDTH ** -0.5, 0.09375, ((1, 4),)),
        "conv_weight": bell_draw(key_of[4], (LAYER_COUNT, CONV_TAPS, INNER_WIDTH), 0.5, 3.0, ((2, 4),)),
        "conv_vec": bell_draw(key_of[5], (LAYER_COUNT, 2, CONV_TAPS, VEC_WIDTH), 0.5, 3.0, ((3, 4),)),
        "conv_state": bell_draw(part_splits[6], (LAYER_COUNT, BATCH_SEQS, CONV_TAPS - 1, INNER_WIDTH), 1.0, 6.0, ((1, 4), (3, 4))),
        "vec_state": bell_draw(part_splits[7], (LAYER_COUNT, 2, BATCH_SEQS, CONV_TAPS - 1, VEC_WIDTH), 1.0, 6.0, ((2, 4), (4, 4))),
        "ssm_state": bell_draw(part_splits[8], (LAYER_COUNT, BATCH_SEQS, HEAD_COUNT, HEAD_DIM, STATE_DIM), 0.5, 4.0, ((1, 4), (2, 4)), jnp.float32),
        "step_bias": jnp.clip(-1.5 + 2.5 * jax.random.uniform(key_of[9], (LAYER_COUNT, HEAD_COUNT), jnp.float32) ** levels(key_of[9], (LAYER_COUNT, HEAD_COUNT), ((1, 4),), -0.2, 0.2), -1.5, 1.0),
        "decay_log": jnp.clip(-4.0 + 5.0 * jax.random.uniform(key_of[10], (LAYER_COUNT, HEAD_COUNT), jnp.float32) ** levels(key_of[10], (LAYER_COUNT, HEAD_COUNT), ((1, 4),), -0.2, 0.2), -4.0, 1.0),
        "skip_gain": jnp.clip(0.5 + 2.5 * jax.random.uniform(key_of[11], (LAYER_COUNT, HEAD_COUNT), jnp.float32) ** levels(key_of[11], (LAYER_COUNT, HEAD_COUNT), ((1, 4),), -0.2, 0.2), 0.5, 3.0),
        "mix_gain": jnp.clip(1.0 + 0.18 * jax.random.normal(key_of[12], (LAYER_COUNT, MODEL_WIDTH), jnp.float32), 0.099609375, 1.8984375).astype(jnp.bfloat16),
        "out_gain": jnp.clip(1.0 + 0.18 * jax.random.normal(key_of[13], (LAYER_COUNT, INNER_WIDTH), jnp.float32), 0.099609375, 1.8984375).astype(jnp.bfloat16),
        "w_out": bell_draw(key_of[14], (LAYER_COUNT, INNER_WIDTH, MODEL_WIDTH), INNER_WIDTH ** -0.5, 0.0625, ((1, 4), (2, 4))),
    }


EPS = 1e-06

def mixer(current, layer, w_in, w_vec, w_step, conv_weight, conv_vec, conv_state, vec_state, ssm_state, step_bias, decay_log, skip_gain, mix_gain, out_gain, w_out):
    batch = current.shape[0]
    xf = current.astype(jnp.float32)
    scale = lax.rsqrt(lax.optimization_barrier(jnp.mean(xf * xf, axis=1)) + EPS)
    scaled_in = (xf * mix_gain[layer].astype(jnp.float32)).astype(jnp.bfloat16)
    proj = jnp.einsum('bd,rdc->brc', scaled_in.astype(jnp.float32), w_in[layer].astype(jnp.float32))
    proj = (proj * scale[:, None, None]).astype(jnp.bfloat16)
    vecs = jnp.einsum('bd,rdc->brc', scaled_in.astype(jnp.float32), w_vec[layer].astype(jnp.float32))
    vecs = (vecs * scale[:, None, None]).astype(jnp.bfloat16)
    step_raw = jnp.dot(scaled_in, w_step[layer], preferred_element_type=jnp.float32) * scale[:, None]
    window = jnp.concatenate([conv_state[layer], proj[:, 1][:, None, :]], axis=1)
    new_conv = window[:, 1:, :]
    values_sum = lax.optimization_barrier(jnp.sum(window.astype(jnp.float32) * conv_weight[layer].astype(jnp.float32)[None, :, :], axis=1))
    fresh = jnp.transpose(vecs, (1, 0, 2))[:, :, None, :]
    vec_window = jnp.concatenate([vec_state[layer], fresh], axis=2)
    new_vec = vec_window[:, :, 1:, :]
    vec_sum = lax.optimization_barrier(jnp.sum(vec_window.astype(jnp.float32) * conv_vec[layer].astype(jnp.float32)[:, None, :, :], axis=2))
    values = jax.nn.silu(values_sum).reshape(batch, HEAD_COUNT, HEAD_DIM)
    vec_act = jax.nn.silu(vec_sum)
    repeat = HEAD_COUNT // GROUP_COUNT
    in_vec = jnp.repeat(vec_act[0].reshape(batch, GROUP_COUNT, STATE_DIM), repeat, axis=1)
    out_vec = jnp.repeat(vec_act[1].reshape(batch, GROUP_COUNT, STATE_DIM), repeat, axis=1)
    step = jax.nn.softplus(step_raw + step_bias[layer][None, :])
    decay = jnp.exp(-step * jnp.exp(decay_log[layer])[None, :])
    state = decay[:, :, None, None] * ssm_state[layer] + (step[:, :, None] * values)[..., None] * in_vec[:, :, None, :]
    read = jnp.einsum('bhpn,bhn->bhp', state, out_vec) + skip_gain[layer][None, :, None] * values
    mixed = read.reshape(batch, INNER_WIDTH) * jax.nn.silu(proj[:, 0].astype(jnp.float32))
    grouped = mixed.reshape(batch, GROUP_COUNT, INNER_WIDTH // GROUP_COUNT)
    grouped = grouped * lax.rsqrt(lax.optimization_barrier(jnp.mean(grouped * grouped, axis=2, keepdims=True)) + EPS)
    normed = (grouped.reshape(batch, INNER_WIDTH) * out_gain[layer].astype(jnp.float32)).astype(jnp.bfloat16)
    result = (xf + jnp.dot(normed, w_out[layer], preferred_element_type=jnp.float32)).astype(jnp.bfloat16)
    return (result, new_conv, new_vec, state)

def reference(tokens, w_in, w_vec, w_step, conv_weight, conv_vec, conv_state, vec_state, ssm_state, step_bias, decay_log, skip_gain, mix_gain, out_gain, w_out):
    current = tokens
    convs = []
    vec_rows = []
    states = []
    for layer in range(LAYER_COUNT):
        current, conv_next, vec_next, state_next = mixer(current, layer, w_in, w_vec, w_step, conv_weight, conv_vec, conv_state, vec_state, ssm_state, step_bias, decay_log, skip_gain, mix_gain, out_gain, w_out)
        convs.append(conv_next)
        vec_rows.append(vec_next)
        states.append(state_next)
    return (current, jnp.stack(convs), jnp.stack(vec_rows), jnp.stack(states))
```

```python
import functools

import jax
import jax.numpy as jnp
from jax import lax
from jax.experimental import pallas as pl
from jax.experimental.pallas import tpu as pltpu
from jax.sharding import PartitionSpec as P

HEAD_DIM = 64
STATE_DIM = 128
LAYER_COUNT = 2
LANES = 128
EPS = 1e-06
VMEM_LIMIT = 56 * 1024 * 1024
DIRECT = 4

F32 = jnp.float32
BF16 = jnp.bfloat16


VMEM = functools.partial(pl.BlockSpec, memory_space=pltpu.VMEM)
ANY = functools.partial(pl.BlockSpec, memory_space=pl.ANY)


def silu(v):
    return v / (1.0 + jnp.exp(-v))


def shift_perm(n, s):
    return [(i, (i + s) % n) for i in range(n)]


def gather_pieces(x, axis, n):
    return [x] + [lax.ppermute(x, axis, shift_perm(n, s)) for s in range(1, n)]


def exchange_pieces(pieces, axis, n):
    return [pieces[0]] + [
        lax.ppermute(pieces[s], axis, shift_perm(n, s)) for s in range(1, n)
    ]


def in_project(layer, stream, partials, mix_gain, w_in, w_vec, w_step, dp, tp, local_heads):
    n_s, n_p = len(stream), len(partials)
    rows, depth = stream[0].shape
    batch = rows * n_s
    part_rows = batch // dp
    own_rows = batch // tp
    cols, vcols = w_in.shape[3], w_vec.shape[3]
    heads = w_step.shape[2]
    width = 2 * cols + 2 * vcols + LANES
    cut = min(512, cols)
    give_own = own_rows % 8 == 0
    chunks = [(1, c) for c in range(0, cols, cut)] + [(0, c) for c in range(0, cols, cut)]

    def kernel(*refs):
        s_refs = refs[:n_s]
        p_refs = refs[n_s : n_s + n_p]
        gain_ref, win, wvec, wstep = refs[n_s + n_p : n_s + n_p + 4]
        outs = refs[n_s + n_p + 4 : n_s + n_p + 4 + dp]
        rest = refs[n_s + n_p + 4 + dp :]
        x_out = rest[0]
        own_out = rest[1] if give_own else None
        xs, bi, bv, bs, sem = rest[-5:]
        dmas = [
            pltpu.make_async_copy(wstep.at[layer], bs, sem.at[0]),
            pltpu.make_async_copy(wvec.at[layer, 0], bv.at[0], sem.at[1]),
            pltpu.make_async_copy(wvec.at[layer, 1], bv.at[1], sem.at[2]),
        ]
        for k, (r, c) in enumerate(chunks):
            dmas.append(
                pltpu.make_async_copy(
                    win.at[layer, r, :, pl.ds(c, cut)], bi.at[k], sem.at[3 + k]
                )
            )
        for d in dmas:
            d.start()
        dp_at = lax.axis_index("dp")
        tp_at = lax.axis_index("tp")
        if n_s == 1:
            xv = s_refs[0][...].astype(F32)
            if n_p:
                add = p_refs[0][...].astype(F32)
                for p in p_refs[1:]:
                    add = add + p[...].astype(F32)
                xv = (xv + add).astype(BF16).astype(F32)
            xs[...] = xv
        else:
            for s in range(n_s):
                at = pl.multiple_of(lax.rem(tp_at - s + n_s, n_s) * rows, 8)
                xs[pl.ds(at, rows), :] = s_refs[s][...].astype(F32)
        x_out[...] = xs[...].astype(BF16)
        if give_own:
            own_out[...] = xs[pl.ds(pl.multiple_of(tp_at * own_rows, 8), own_rows), :].astype(BF16)
        blocks = []
        for s in range(dp):
            at = pl.multiple_of(lax.rem(dp_at + s, dp) * part_rows, 8)
            blocks.append(xs[pl.ds(at, part_rows), :])
        x = jnp.concatenate(blocks, axis=0)
        sq = jnp.sum(x * x, axis=1, keepdims=True)
        lhs = (x * gain_ref[layer : layer + 1, :].astype(F32)).astype(BF16)

        def put(col, res):
            res = res.astype(BF16)
            for s in range(dp):
                outs[s][:, col : col + res.shape[1]] = res[s * part_rows : (s + 1) * part_rows]

        dmas[0].wait()
        step = jnp.dot(lhs, bs[...], preferred_element_type=F32).astype(BF16)
        i_at = lax.broadcasted_iota(jnp.int32, (heads, LANES), 0)
        j_at = lax.broadcasted_iota(jnp.int32, (heads, LANES), 1)
        pick = (i_at == j_at + tp_at * local_heads) & (j_at < local_heads)
        step = jnp.dot(step, pick.astype(F32).astype(BF16), preferred_element_type=F32)
        lane = lax.broadcasted_iota(jnp.int32, (batch, LANES), 1)
        high = sq.astype(BF16).astype(F32)
        tail = jnp.where(lane == local_heads, high, step)
        tail = jnp.where(lane == local_heads + 1, sq - high, tail)
        put(2 * cols + 2 * vcols, tail)
        for r in range(2):
            dmas[1 + r].wait()
            put(2 * cols + r * vcols, jnp.dot(lhs, bv[r], preferred_element_type=F32))
        for k, (r, c) in enumerate(chunks):
            dmas[3 + k].wait()
            put(r * cols + c, jnp.dot(lhs, bi[k], preferred_element_type=F32))

    out_shape = [jax.ShapeDtypeStruct((part_rows, width), BF16)] * dp
    out_shape.append(jax.ShapeDtypeStruct((batch, depth), BF16))
    if give_own:
        out_shape.append(jax.ShapeDtypeStruct((own_rows, depth), BF16))
    res = pl.pallas_call(
        kernel,
        out_shape=out_shape,
        in_specs=[VMEM()] * (n_s + n_p + 1) + [ANY()] * 3,
        out_specs=[VMEM()] * len(out_shape),
        scratch_shapes=[
            pltpu.VMEM((batch, depth), F32),
            pltpu.VMEM((len(chunks), depth, cut), BF16),
            pltpu.VMEM((2, depth, vcols), BF16),
            pltpu.VMEM((depth, heads), BF16),
            pltpu.SemaphoreType.DMA((3 + len(chunks),)),
        ],
        compiler_params=pltpu.CompilerParams(vmem_limit_bytes=VMEM_LIMIT),
        name="in_project",
    )(*stream, *partials, mix_gain, w_in, w_vec, w_step)
    return res[:dp], res[dp], res[dp + 1] if give_own else None


def mix(layer, sums, model_width, conv_weight, conv_vec, conv_state, vec_state, ssm_state,
        step_bias, decay_log, skip, out_gain, previous):
    n = len(sums)
    rows = sums[0].shape[0]
    cols, vcols = conv_weight.shape[2], conv_vec.shape[3]
    hl = ssm_state.shape[2]
    groups = vcols // STATE_DIM
    rep = hl // groups
    span = cols // groups
    tail = 2 * cols + 2 * vcols
    slabs = cols // LANES
    slab_pad = -(-slabs // 8) * 8
    per = LANES // HEAD_DIM

    def kernel(*refs):
        s_refs = refs[:n]
        cw, cv, cs, vs, ssm, bias, dlog, skip_ref, og = refs[n : n + 9]
        rest = refs[n + 9 + len(previous) :]
        normed, ncs, nvs, nssm = rest[:4]
        vt, val_s, gate_s, in_s, out_s, dt_s, dec_s, read_s = rest[4:]
        b = pl.program_id(0)

        @pl.when(b == 0)
        def _():
            def total(lo, hi):
                t = s_refs[0][:, lo:hi].astype(F32)
                for s in s_refs[1:]:
                    t = t + s[:, lo:hi].astype(F32)
                return t

            end = total(tail, tail + LANES)
            own_sq = end[:, hl : hl + 1] + end[:, hl + 1 : hl + 2]
            scale = lax.rsqrt(own_sq / model_width + EPS)
            z = end[:, :hl] * scale + bias[layer : layer + 1, :]
            dt = jnp.maximum(z, 0.0) + jnp.log1p(jnp.exp(-jnp.abs(z)))
            dt_s[:, 0, :] = dt
            dec_s[:, 0, :] = jnp.exp(-dt * jnp.exp(dlog[layer : layer + 1, :]))
            for r in range(2):
                fresh = (total(2 * cols + r * vcols, 2 * cols + (r + 1) * vcols) * scale).astype(BF16)
                acc = fresh.astype(F32) * cv[0, r, 3:4, :].astype(F32)
                for i in range(3):
                    acc = acc + vs[0, r, i].astype(F32) * cv[0, r, i : i + 1, :].astype(F32)
                nvs[0, r, 0] = vs[0, r, 1]
                nvs[0, r, 1] = vs[0, r, 2]
                nvs[0, r, 2] = fresh
                acc = silu(acc)
                for g in range(groups):
                    (in_s if r == 0 else out_s)[:, g, :] = acc[:, g * STATE_DIM : (g + 1) * STATE_DIM]
            gate = (total(0, cols) * scale).astype(BF16).astype(F32)
            gate_s[...] = silu(gate)
            fresh = (total(cols, 2 * cols) * scale).astype(BF16)
            acc = fresh.astype(F32) * cw[0, 3:4, :].astype(F32)
            for i in range(3):
                acc = acc + cs[0, i].astype(F32) * cw[0, i : i + 1, :].astype(F32)
            ncs[0, 0] = cs[0, 1]
            ncs[0, 1] = cs[0, 2]
            ncs[0, 2] = fresh
            values = silu(acc)
            val_s[...] = values
            for j in range(slabs):
                vt[:, j, :] = values[:, j * LANES : (j + 1) * LANES]

        turned = vt[b].T
        dt_row = dt_s[b]
        dec_row = dec_s[b]
        in_rows = in_s[b]
        out_rows = out_s[b]
        for g in range(groups):
            in_row = in_rows[g : g + 1]
            out_row = out_rows[g : g + 1]
            states = []
            for k in range(rep):
                h = g * rep + k
                at = (h % per) * HEAD_DIM
                col = turned[at : at + HEAD_DIM, h // per : h // per + 1]
                st = ssm[0, 0, h] * dec_row[:, h : h + 1] + col * (in_row * dt_row[:, h : h + 1])
                nssm[0, 0, h] = st
                states.append(st.astype(BF16))
            whole = jnp.concatenate(states, axis=0)
            got = lax.dot_general(
                jnp.broadcast_to(out_row, (8, STATE_DIM)).astype(BF16),
                whole,
                (((1,), (1,)), ((), ())),
                preferred_element_type=F32,
            )
            read_s[b, g : g + 1, :] = got[0:1]

        @pl.when(b == rows - 1)
        def _():
            for g in range(groups):
                at = slice(g * span, (g + 1) * span)
                m = (read_s[:, g, :] + skip_ref[layer : layer + 1, at] * val_s[:, at]) * gate_s[:, at]
                m = m * lax.rsqrt(jnp.mean(m * m, axis=1, keepdims=True) + EPS)
                normed[:, at] = (m * og[layer : layer + 1, at].astype(F32)).astype(BF16)

    def layer_block(a):
        nd = a.ndim
        return pl.BlockSpec((1,) + a.shape[1:], lambda b: (layer,) + (0,) * (nd - 1))

    state_spec = pl.BlockSpec((1, 1) + ssm_state.shape[2:], lambda b: (layer, b, 0, 0, 0))
    aliases = {n + 9 + i: 1 + i for i in range(len(previous))}
    return pl.pallas_call(
        kernel,
        grid=(rows,),
        out_shape=[
            jax.ShapeDtypeStruct((rows, cols), BF16),
            jax.ShapeDtypeStruct(conv_state.shape, BF16),
            jax.ShapeDtypeStruct(vec_state.shape, BF16),
            jax.ShapeDtypeStruct(ssm_state.shape, F32),
        ],
        in_specs=[VMEM()] * n
        + [layer_block(conv_weight), layer_block(conv_vec), layer_block(conv_state),
           layer_block(vec_state), state_spec, VMEM(), VMEM(), VMEM(), VMEM()]
        + [ANY()] * len(previous),
        out_specs=[
            pl.BlockSpec((rows, cols), lambda b: (0, 0)),
            layer_block(conv_state),
            layer_block(vec_state),
            state_spec,
        ],
        scratch_shapes=[
            pltpu.VMEM((rows, slab_pad, LANES), F32),
            pltpu.VMEM((rows, cols), F32),
            pltpu.VMEM((rows, cols), F32),
            pltpu.VMEM((rows, groups, STATE_DIM), F32),
            pltpu.VMEM((rows, groups, STATE_DIM), F32),
            pltpu.VMEM((rows, 1, hl), F32),
            pltpu.VMEM((rows, 1, hl), F32),
            pltpu.VMEM((rows, groups, span), F32),
        ],
        input_output_aliases=aliases,
        compiler_params=pltpu.CompilerParams(
            vmem_limit_bytes=VMEM_LIMIT, dimension_semantics=("arbitrary",)
        ),
        name="mix",
    )(*sums, conv_weight, conv_vec, conv_state, vec_state, ssm_state, step_bias, decay_log,
      skip, out_gain, *previous)


def out_project(layer, pieces, w_out, dp, tp, scatter):
    n = len(pieces)
    rows = pieces[0].shape[0]
    batch = rows * n
    depth, width = w_out.shape[1], w_out.shape[2]
    cut = min(512, depth)
    steps = depth // cut
    n_out = tp if scatter else 1
    out_rows = batch // n_out

    def kernel(*refs):
        p_refs = refs[:n]
        w = refs[n]
        outs = refs[n + 1 : n + 1 + n_out]
        acc, buf, sem = refs[n + 1 + n_out :]
        dmas = [
            pltpu.make_async_copy(w.at[layer, pl.ds(k * cut, cut)], buf.at[k], sem.at[k])
            for k in range(steps)
        ]
        for d in dmas:
            d.start()
        lhs = jnp.concatenate([p[...] for p in p_refs], axis=0)
        res = None
        for k in range(steps):
            dmas[k].wait()
            t = jnp.dot(lhs[:, k * cut : (k + 1) * cut], buf[k], preferred_element_type=F32)
            res = t if res is None else res + t
        if n == 1:
            acc[...] = res
        else:
            dp_at = lax.axis_index("dp")
            for s in range(n):
                at = pl.multiple_of(lax.rem(dp_at - s + n, n) * rows, 8)
                acc[pl.ds(at, rows), :] = res[s * rows : (s + 1) * rows]
        if n_out == 1:
            outs[0][...] = acc[...].astype(BF16)
        else:
            tp_at = lax.axis_index("tp")
            for s in range(n_out):
                at = pl.multiple_of(lax.rem(tp_at + s, n_out) * out_rows, 8)
                outs[s][...] = acc[pl.ds(at, out_rows), :].astype(BF16)

    return pl.pallas_call(
        kernel,
        out_shape=[jax.ShapeDtypeStruct((out_rows, width), BF16)] * n_out,
        in_specs=[VMEM()] * n + [ANY()],
        out_specs=[VMEM()] * n_out,
        scratch_shapes=[
            pltpu.VMEM((batch, width), F32),
            pltpu.VMEM((steps, cut, width), BF16),
            pltpu.SemaphoreType.DMA((steps,)),
        ],
        compiler_params=pltpu.CompilerParams(vmem_limit_bytes=VMEM_LIMIT),
        name="out_project",
    )(*pieces, w_out)


def shards(dp, tp, tokens, w_in, w_vec, w_step, conv_weight, conv_vec, conv_state, vec_state,
           ssm_state, step_bias, decay_log, skip_gain, mix_gain, out_gain, w_out):
    own_rows, depth = tokens.shape
    direct_dp = dp <= DIRECT
    direct_tp = tp <= DIRECT and own_rows % 8 == 0
    local_heads = ssm_state.shape[2]
    conv_rows = jnp.transpose(conv_state, (0, 2, 1, 3))
    vec_rows = jnp.transpose(vec_state, (0, 1, 3, 2, 4))
    skip = jnp.repeat(skip_gain, HEAD_DIM, axis=1)
    if direct_tp:
        stream = gather_pieces(tokens, "tp", tp)
    else:
        stream = [lax.all_gather(tokens, "tp", axis=0, tiled=True)]
    partials = []
    previous = ()
    own = tokens
    for layer in range(LAYER_COUNT):
        last = layer == LAYER_COUNT - 1
        blocks, whole, own = in_project(
            layer, stream, partials, mix_gain, w_in, w_vec, w_step, dp, tp, local_heads
        )
        if own is None:
            own = lax.dynamic_slice_in_dim(whole, lax.axis_index("tp") * own_rows, own_rows, 0)
        if direct_dp:
            sums = exchange_pieces(blocks, "dp", dp)
        else:
            got = lax.all_to_all(rotate_back(blocks, dp), "dp", 0, 0, tiled=True)
            sums = [jnp.sum(got.astype(F32), axis=0)]
        normed, *previous = mix(
            layer, sums, float(depth * dp), conv_weight, conv_vec, conv_rows, vec_rows,
            ssm_state, step_bias, decay_log, skip, out_gain, previous,
        )
        if direct_dp:
            pieces = gather_pieces(normed, "dp", dp)
        else:
            pieces = [lax.all_gather(normed, "dp", axis=0, tiled=True)]
        outs = out_project(layer, pieces, w_out, dp, tp, last and direct_tp)
        stream = [whole]
        if not last:
            if direct_tp:
                partials = gather_pieces(outs[0], "tp", tp)
            else:
                partials = [lax.psum(outs[0], "tp")]
    if direct_tp:
        got = exchange_pieces(outs, "tp", tp)
        add = sum(g.astype(F32) for g in got)
    else:
        add = lax.psum_scatter(outs[0], "tp", scatter_dimension=0, tiled=True).astype(F32)
    result = (own.astype(F32) + add).astype(BF16)
    new_conv, new_vec, new_ssm = previous
    return (
        result,
        jnp.transpose(new_conv, (0, 2, 1, 3)),
        jnp.transpose(new_vec, (0, 1, 3, 2, 4)),
        new_ssm,
    )


def rotate_back(blocks, n):
    return jnp.roll(jnp.stack(blocks), lax.axis_index("dp"), axis=0)


def solution(mesh):
    placed = (
        P(("grp", "tp"), "dp"),
        P(None, None, "dp", "tp"),
        P(None, None, "dp", "tp"),
        P(None, "dp", None),
        P(None, None, "tp"),
        P(None, None, None, "tp"),
        P(None, ("grp", "dp"), None, "tp"),
        P(None, None, ("grp", "dp"), None, "tp"),
        P(None, ("grp", "dp"), "tp", None, None),
        P(None, "tp"),
        P(None, "tp"),
        P(None, "tp"),
        P(None, "dp"),
        P(None, "tp"),
        P(None, "tp", "dp"),
    )
    return jax.shard_map(
        functools.partial(shards, mesh.shape["dp"], mesh.shape["tp"]),
        mesh=mesh,
        in_specs=placed,
        out_specs=(
            P(("grp", "tp"), "dp"),
            P(None, ("grp", "dp"), None, "tp"),
            P(None, None, ("grp", "dp"), None, "tp"),
            P(None, ("grp", "dp"), "tp", None, None),
        ),
        check_vma=False,
    )
```

```python
import functools

import jax
import jax.numpy as jnp
from jax import lax
from jax.experimental import pallas as pl
from jax.experimental.pallas import tpu as pltpu
from jax.sharding import PartitionSpec as P

HEAD_DIM = 64
STATE_DIM = 128
LAYER_COUNT = 2
LANES = 128
EPS = 1e-06
VMEM_LIMIT = 16 * 1024 * 1024
DIRECT = 4

F32 = jnp.float32
BF16 = jnp.bfloat16


VMEM = functools.partial(pl.BlockSpec, memory_space=pltpu.VMEM)
ANY = functools.partial(pl.BlockSpec, memory_space=pl.ANY)


def silu(v):
    return v / (1.0 + jnp.exp(-v))


def shift_perm(n, s):
    return [(i, (i + s) % n) for i in range(n)]


def gather_pieces(x, axis, n):
    return [x] + [lax.ppermute(x, axis, shift_perm(n, s)) for s in range(1, n)]


def exchange_pieces(pieces, axis, n):
    return [pieces[0]] + [
        lax.ppermute(pieces[s], axis, shift_perm(n, s)) for s in range(1, n)
    ]


def in_project(layer, stream, partials, mix_gain, w_in, w_vec, w_step, dp, tp, local_heads):
    n_s, n_p = len(stream), len(partials)
    rows, depth = stream[0].shape
    batch = rows * n_s
    part_rows = batch // dp
    own_rows = batch // tp
    cols, vcols = w_in.shape[3], w_vec.shape[3]
    heads = w_step.shape[2]
    width = 2 * cols + 2 * vcols + LANES
    cut = min(512, cols)
    give_own = own_rows % 8 == 0
    chunks = [(1, c) for c in range(0, cols, cut)] + [(0, c) for c in range(0, cols, cut)]

    def kernel(*refs):
        s_refs = refs[:n_s]
        p_refs = refs[n_s : n_s + n_p]
        gain_ref, win, wvec, wstep = refs[n_s + n_p : n_s + n_p + 4]
        outs = refs[n_s + n_p + 4 : n_s + n_p + 4 + dp]
        rest = refs[n_s + n_p + 4 + dp :]
        x_out = rest[0]
        own_out = rest[1] if give_own else None
        xs, bi, bv, bs, sem = rest[-5:]
        dmas = [
            pltpu.make_async_copy(wstep.at[layer], bs, sem.at[0]),
            pltpu.make_async_copy(wvec.at[layer, 0], bv.at[0], sem.at[1]),
            pltpu.make_async_copy(wvec.at[layer, 1], bv.at[1], sem.at[2]),
        ]
        for k, (r, c) in enumerate(chunks):
            dmas.append(
                pltpu.make_async_copy(
                    win.at[layer, r, :, pl.ds(c, cut)], bi.at[k], sem.at[3 + k]
                )
            )
        for d in dmas:
            d.start()
        dp_at = lax.axis_index("dp")
        tp_at = lax.axis_index("tp")
        if n_s == 1:
            xv = s_refs[0][...].astype(F32)
            if n_p:
                add = p_refs[0][...].astype(F32)
                for p in p_refs[1:]:
                    add = add + p[...].astype(F32)
                xv = (xv + add).astype(BF16).astype(F32)
            xs[...] = xv
        else:
            for s in range(n_s):
                at = pl.multiple_of(lax.rem(tp_at - s + n_s, n_s) * rows, 8)
                xs[pl.ds(at, rows), :] = s_refs[s][...].astype(F32)
        x_out[...] = xs[...].astype(BF16)
        if give_own:
            own_out[...] = xs[pl.ds(pl.multiple_of(tp_at * own_rows, 8), own_rows), :].astype(BF16)
        blocks = []
        for s in range(dp):
            at = pl.multiple_of(lax.rem(dp_at + s, dp) * part_rows, 8)
            blocks.append(xs[pl.ds(at, part_rows), :])
        x = jnp.concatenate(blocks, axis=0)
        sq = jnp.sum(x * x, axis=1, keepdims=True)
        lhs = (x * gain_ref[layer : layer + 1, :].astype(F32)).astype(BF16)

        def put(col, res):
            res = res.astype(BF16)
            for s in range(dp):
                outs[s][:, col : col + res.shape[1]] = res[s * part_rows : (s + 1) * part_rows]

        dmas[0].wait()
        step = jnp.dot(lhs, bs[...], preferred_element_type=F32).astype(BF16)
        i_at = lax.broadcasted_iota(jnp.int32, (heads, LANES), 0)
        j_at = lax.broadcasted_iota(jnp.int32, (heads, LANES), 1)
        pick = (i_at == j_at + tp_at * local_heads) & (j_at < local_heads)
        step = jnp.dot(step, pick.astype(F32).astype(BF16), preferred_element_type=F32)
        lane = lax.broadcasted_iota(jnp.int32, (batch, LANES), 1)
        high = sq.astype(BF16).astype(F32)
        tail = jnp.where(lane == local_heads, high, step)
        tail = jnp.where(lane == local_heads + 1, sq - high, tail)
        put(2 * cols + 2 * vcols, tail)
        for r in range(2):
            dmas[1 + r].wait()
            put(2 * cols + r * vcols, jnp.dot(lhs, bv[r], preferred_element_type=F32))
        for k, (r, c) in enumerate(chunks):
            dmas[3 + k].wait()
            put(r * cols + c, jnp.dot(lhs, bi[k], preferred_element_type=F32))

    out_shape = [jax.ShapeDtypeStruct((part_rows, width), BF16)] * dp
    out_shape.append(jax.ShapeDtypeStruct((batch, depth), BF16))
    if give_own:
        out_shape.append(jax.ShapeDtypeStruct((own_rows, depth), BF16))
    res = pl.pallas_call(
        kernel,
        out_shape=out_shape,
        in_specs=[VMEM()] * (n_s + n_p + 1) + [ANY()] * 3,
        out_specs=[VMEM()] * len(out_shape),
        scratch_shapes=[
            pltpu.VMEM((batch, depth), F32),
            pltpu.VMEM((len(chunks), depth, cut), BF16),
            pltpu.VMEM((2, depth, vcols), BF16),
            pltpu.VMEM((depth, heads), BF16),
            pltpu.SemaphoreType.DMA((3 + len(chunks),)),
        ],
        compiler_params=pltpu.CompilerParams(vmem_limit_bytes=VMEM_LIMIT),
        name="in_project",
    )(*stream, *partials, mix_gain, *(pltpu.with_memory_space_constraint(w, pltpu.HBM) for w in (w_in, w_vec, w_step)))
    return res[:dp], res[dp], res[dp + 1] if give_own else None


def mix(layer, sums, model_width, conv_weight, conv_vec, conv_state, vec_state, ssm_state,
        step_bias, decay_log, skip, out_gain, previous):
    n = len(sums)
    rows = sums[0].shape[0]
    cols, vcols = conv_weight.shape[2], conv_vec.shape[3]
    hl = ssm_state.shape[2]
    groups = vcols // STATE_DIM
    rep = hl // groups
    span = cols // groups
    tail = 2 * cols + 2 * vcols
    slabs = cols // LANES
    slab_pad = -(-slabs // 8) * 8
    per = LANES // HEAD_DIM

    def kernel(*refs):
        s_refs = refs[:n]
        cw, cv, cs, vs, ssm, bias, dlog, skip_ref, og = refs[n : n + 9]
        rest = refs[n + 9 + len(previous) :]
        normed, ncs, nvs, nssm = rest[:4]
        vt, val_s, gate_s, in_s, out_s, dt_s, dec_s, read_s = rest[4:]
        b = pl.program_id(0)

        @pl.when(b == 0)
        def _():
            def total(lo, hi):
                t = s_refs[0][:, lo:hi].astype(F32)
                for s in s_refs[1:]:
                    t = t + s[:, lo:hi].astype(F32)
                return t

            end = total(tail, tail + LANES)
            own_sq = end[:, hl : hl + 1] + end[:, hl + 1 : hl + 2]
            scale = lax.rsqrt(own_sq / model_width + EPS)
            z = end[:, :hl] * scale + bias[layer : layer + 1, :]
            dt = jnp.maximum(z, 0.0) + jnp.log1p(jnp.exp(-jnp.abs(z)))
            dt_s[:, 0, :] = dt
            dec_s[:, 0, :] = jnp.exp(-dt * jnp.exp(dlog[layer : layer + 1, :]))
            for r in range(2):
                fresh = (total(2 * cols + r * vcols, 2 * cols + (r + 1) * vcols) * scale).astype(BF16)
                acc = fresh.astype(F32) * cv[0, r, 3:4, :].astype(F32)
                for i in range(3):
                    acc = acc + vs[0, r, i].astype(F32) * cv[0, r, i : i + 1, :].astype(F32)
                nvs[0, r, 0] = vs[0, r, 1]
                nvs[0, r, 1] = vs[0, r, 2]
                nvs[0, r, 2] = fresh
                acc = silu(acc)
                for g in range(groups):
                    (in_s if r == 0 else out_s)[:, g, :] = acc[:, g * STATE_DIM : (g + 1) * STATE_DIM]
            gate = (total(0, cols) * scale).astype(BF16).astype(F32)
            gate_s[...] = silu(gate)
            fresh = (total(cols, 2 * cols) * scale).astype(BF16)
            acc = fresh.astype(F32) * cw[0, 3:4, :].astype(F32)
            for i in range(3):
                acc = acc + cs[0, i].astype(F32) * cw[0, i : i + 1, :].astype(F32)
            ncs[0, 0] = cs[0, 1]
            ncs[0, 1] = cs[0, 2]
            ncs[0, 2] = fresh
            values = silu(acc)
            val_s[...] = values
            for j in range(slabs):
                vt[:, j, :] = values[:, j * LANES : (j + 1) * LANES]

        turned = vt[b].T
        dt_row = dt_s[b]
        dec_row = dec_s[b]
        in_rows = in_s[b]
        out_rows = out_s[b]
        for g in range(groups):
            in_row = in_rows[g : g + 1]
            out_row = out_rows[g : g + 1]
            states = []
            for k in range(rep):
                h = g * rep + k
                at = (h % per) * HEAD_DIM
                col = turned[at : at + HEAD_DIM, h // per : h // per + 1]
                st = ssm[0, 0, h] * dec_row[:, h : h + 1] + col * (in_row * dt_row[:, h : h + 1])
                nssm[0, 0, h] = st
                states.append(st.astype(BF16))
            whole = jnp.concatenate(states, axis=0)
            got = lax.dot_general(
                jnp.broadcast_to(out_row, (8, STATE_DIM)).astype(BF16),
                whole,
                (((1,), (1,)), ((), ())),
                preferred_element_type=F32,
            )
            read_s[b, g : g + 1, :] = got[0:1]

        @pl.when(b == rows - 1)
        def _():
            for g in range(groups):
                at = slice(g * span, (g + 1) * span)
                m = (read_s[:, g, :] + skip_ref[layer : layer + 1, at] * val_s[:, at]) * gate_s[:, at]
                m = m * lax.rsqrt(jnp.mean(m * m, axis=1, keepdims=True) + EPS)
                normed[:, at] = (m * og[layer : layer + 1, at].astype(F32)).astype(BF16)

    def layer_block(a):
        nd = a.ndim
        return pl.BlockSpec((1,) + a.shape[1:], lambda b: (layer,) + (0,) * (nd - 1))

    state_spec = pl.BlockSpec((1, 1) + ssm_state.shape[2:], lambda b: (layer, b, 0, 0, 0))
    aliases = {n + 9 + i: 1 + i for i in range(len(previous))}
    return pl.pallas_call(
        kernel,
        grid=(rows,),
        out_shape=[
            jax.ShapeDtypeStruct((rows, cols), BF16),
            jax.ShapeDtypeStruct(conv_state.shape, BF16),
            jax.ShapeDtypeStruct(vec_state.shape, BF16),
            jax.ShapeDtypeStruct(ssm_state.shape, F32),
        ],
        in_specs=[VMEM()] * n
        + [layer_block(conv_weight), layer_block(conv_vec), layer_block(conv_state),
           layer_block(vec_state), state_spec, VMEM(), VMEM(), VMEM(), VMEM()]
        + [ANY()] * len(previous),
        out_specs=[
            pl.BlockSpec((rows, cols), lambda b: (0, 0)),
            layer_block(conv_state),
            layer_block(vec_state),
            state_spec,
        ],
        scratch_shapes=[
            pltpu.VMEM((rows, slab_pad, LANES), F32),
            pltpu.VMEM((rows, cols), F32),
            pltpu.VMEM((rows, cols), F32),
            pltpu.VMEM((rows, groups, STATE_DIM), F32),
            pltpu.VMEM((rows, groups, STATE_DIM), F32),
            pltpu.VMEM((rows, 1, hl), F32),
            pltpu.VMEM((rows, 1, hl), F32),
            pltpu.VMEM((rows, groups, span), F32),
        ],
        input_output_aliases=aliases,
        compiler_params=pltpu.CompilerParams(
            vmem_limit_bytes=VMEM_LIMIT, dimension_semantics=("arbitrary",)
        ),
        name="mix",
    )(*sums, conv_weight, conv_vec, conv_state, vec_state, ssm_state, step_bias, decay_log,
      skip, out_gain, *previous)


def out_project(layer, pieces, w_out, dp, tp, scatter):
    n = len(pieces)
    rows = pieces[0].shape[0]
    batch = rows * n
    depth, width = w_out.shape[1], w_out.shape[2]
    cut = min(512, depth)
    steps = depth // cut
    n_out = tp if scatter else 1
    out_rows = batch // n_out

    def kernel(*refs):
        p_refs = refs[:n]
        w = refs[n]
        outs = refs[n + 1 : n + 1 + n_out]
        acc, buf, sem = refs[n + 1 + n_out :]
        dmas = [
            pltpu.make_async_copy(w.at[layer, pl.ds(k * cut, cut)], buf.at[k], sem.at[k])
            for k in range(steps)
        ]
        for d in dmas:
            d.start()
        lhs = jnp.concatenate([p[...] for p in p_refs], axis=0)
        res = None
        for k in range(steps):
            dmas[k].wait()
            t = jnp.dot(lhs[:, k * cut : (k + 1) * cut], buf[k], preferred_element_type=F32)
            res = t if res is None else res + t
        if n == 1:
            acc[...] = res
        else:
            dp_at = lax.axis_index("dp")
            for s in range(n):
                at = pl.multiple_of(lax.rem(dp_at - s + n, n) * rows, 8)
                acc[pl.ds(at, rows), :] = res[s * rows : (s + 1) * rows]
        if n_out == 1:
            outs[0][...] = acc[...].astype(BF16)
        else:
            tp_at = lax.axis_index("tp")
            for s in range(n_out):
                at = pl.multiple_of(lax.rem(tp_at + s, n_out) * out_rows, 8)
                outs[s][...] = acc[pl.ds(at, out_rows), :].astype(BF16)

    return pl.pallas_call(
        kernel,
        out_shape=[jax.ShapeDtypeStruct((out_rows, width), BF16)] * n_out,
        in_specs=[VMEM()] * n + [ANY()],
        out_specs=[VMEM()] * n_out,
        scratch_shapes=[
            pltpu.VMEM((batch, width), F32),
            pltpu.VMEM((steps, cut, width), BF16),
            pltpu.SemaphoreType.DMA((steps,)),
        ],
        compiler_params=pltpu.CompilerParams(vmem_limit_bytes=VMEM_LIMIT),
        name="out_project",
    )(*pieces, w_out)


def shards(dp, tp, tokens, w_in, w_vec, w_step, conv_weight, conv_vec, conv_state, vec_state,
           ssm_state, step_bias, decay_log, skip_gain, mix_gain, out_gain, w_out):
    own_rows, depth = tokens.shape
    direct_dp = dp <= DIRECT
    direct_tp = tp <= DIRECT and own_rows % 8 == 0
    local_heads = ssm_state.shape[2]
    conv_rows = jnp.transpose(conv_state, (0, 2, 1, 3))
    vec_rows = jnp.transpose(vec_state, (0, 1, 3, 2, 4))
    skip = jnp.repeat(skip_gain, HEAD_DIM, axis=1)
    if direct_tp:
        stream = gather_pieces(tokens, "tp", tp)
    else:
        stream = [lax.all_gather(tokens, "tp", axis=0, tiled=True)]
    partials = []
    previous = ()
    own = tokens
    for layer in range(LAYER_COUNT):
        last = layer == LAYER_COUNT - 1
        blocks, whole, own = in_project(
            layer, stream, partials, mix_gain, w_in, w_vec, w_step, dp, tp, local_heads
        )
        if own is None:
            own = lax.dynamic_slice_in_dim(whole, lax.axis_index("tp") * own_rows, own_rows, 0)
        if direct_dp:
            sums = exchange_pieces(blocks, "dp", dp)
        else:
            got = lax.all_to_all(rotate_back(blocks, dp), "dp", 0, 0, tiled=True)
            sums = [jnp.sum(got.astype(F32), axis=0)]
        normed, *previous = mix(
            layer, sums, float(depth * dp), conv_weight, conv_vec, conv_rows, vec_rows,
            ssm_state, step_bias, decay_log, skip, out_gain, previous,
        )
        if direct_dp:
            pieces = gather_pieces(normed, "dp", dp)
        else:
            pieces = [lax.all_gather(normed, "dp", axis=0, tiled=True)]
        outs = out_project(layer, pieces, w_out, dp, tp, last and direct_tp)
        stream = [whole]
        if not last:
            if direct_tp:
                partials = gather_pieces(outs[0], "tp", tp)
            else:
                partials = [lax.psum(outs[0], "tp")]
    if direct_tp:
        got = exchange_pieces(outs, "tp", tp)
        add = sum(g.astype(F32) for g in got)
    else:
        add = lax.psum_scatter(outs[0], "tp", scatter_dimension=0, tiled=True).astype(F32)
    result = (own.astype(F32) + add).astype(BF16)
    new_conv, new_vec, new_ssm = previous
    return (
        result,
        jnp.transpose(new_conv, (0, 2, 1, 3)),
        jnp.transpose(new_vec, (0, 1, 3, 2, 4)),
        new_ssm,
    )


def rotate_back(blocks, n):
    return jnp.roll(jnp.stack(blocks), lax.axis_index("dp"), axis=0)


def solution(mesh):
    placed = (
        P(("grp", "tp"), "dp"),
        P(None, None, "dp", "tp"),
        P(None, None, "dp", "tp"),
        P(None, "dp", None),
        P(None, None, "tp"),
        P(None, None, None, "tp"),
        P(None, ("grp", "dp"), None, "tp"),
        P(None, None, ("grp", "dp"), None, "tp"),
        P(None, ("grp", "dp"), "tp", None, None),
        P(None, "tp"),
        P(None, "tp"),
        P(None, "tp"),
        P(None, "dp"),
        P(None, "tp"),
        P(None, "tp", "dp"),
    )
    return jax.shard_map(
        functools.partial(shards, mesh.shape["dp"], mesh.shape["tp"]),
        mesh=mesh,
        in_specs=placed,
        out_specs=(
            P(("grp", "tp"), "dp"),
            P(None, ("grp", "dp"), None, "tp"),
            P(None, None, ("grp", "dp"), None, "tp"),
            P(None, ("grp", "dp"), "tp", None, None),
        ),
        check_vma=False,
    )
```
